256 devices in a mesh: grp: 2 (over y), ep: 32 (over z, core), tp: 4 (over x).
Axes of the slice: x: 4, y: 2, z: 16, core: 2. Of those that a mesh axis runs over, the one named last changes fastest.
The devices are a block of a 4x16x16 slice.
Arguments:
- outer_gate: bfloat16 [16384, 2048], P(('grp', 'ep'), 'tp'), parts along dimension 0, may hold values from -6 to 6
- inner_gate: bfloat16 [16384, 2048], P(('grp', 'ep'), 'tp'), parts along dimension 0, may hold values from -6 to 6
- inner_value: bfloat16 [16384, 2048], P(('grp', 'ep'), 'tp'), parts along dimension 0, may hold values from -6 to 6
- conv_taps: bfloat16 [3, 2048], replicated, may hold values from -3 to 3
- mixer_out: bfloat16 [2048, 2048], P('tp'), may hold values from -0.125 to 0.125
- mixer_gain: float32 [2048], replicated, may hold values from 0.1 to 1.9
- moe_tokens: bfloat16 [16384, 2048], P(('grp', 'ep', 'tp')), parts along dimension 0, may hold values from -6 to 6
- expert_gain: float32 [2048], replicated, may hold values from 0.1 to 1.9
- route_ids: int32 [16384, 4], P(('grp', 'ep', 'tp')), parts along dimension 0, may hold values from 0 to 127, all different within a row; in each aligned block of 64 rows (0 to 63, 64 to 127, ...) at most 3 rows name the same one
- route_weights: float32 [16384, 4], P(('grp', 'ep', 'tp')), parts along dimension 0, may hold values from 0.2 to 1
- expert_gate: bfloat16 [128, 2048, 512], P(('ep', 'tp')), may hold values from -0.125 to 0.125
- expert_up: bfloat16 [128, 2048, 512], P(('ep', 'tp')), may hold values from -0.125 to 0.125
- expert_down: bfloat16 [128, 512, 2048], P(('ep', 'tp')), may hold values from -0.25 to 0.25
- shared_gate: bfloat16 [2048, 512], P(None, 'tp'), may hold values from -0.125 to 0.125
- shared_up: bfloat16 [2048, 512], P(None, 'tp'), may hold values from -0.125 to 0.125
- shared_down: bfloat16 [512, 2048], P('tp'), may hold values from -0.25 to 0.25
Outputs:
- mixed_rows: bfloat16 [16384, 2048], P(('grp', 'ep', 'tp')), parts along dimension 0
- expert_rows: bfloat16 [16384, 2048], P(('grp', 'ep', 'tp')), parts along dimension 0
The draws below stay inside these ranges and needn't reach their ends.
There are 2 independent parts, one for each index of `grp`. The reference program is written for one: setup_inputs(seed, part) draws one part's arguments, and reference() takes and returns one part's arrays. A program takes and returns all parts, laid end to end along the dimension named above; an argument that names none is the same for every part. Nothing has to cross between parts.
Inputs may be any that keep to these rules, and one draw needn't show every extreme that they name: `route_ids`: each row names 4 different experts; among the 64 rows of one device (aligned blocks) no expert is named more than 3 times, a bound that some block reaches.
All inputs are finite; a program needn't handle non-finite values.
Results may differ from the reference program's by a relative error of at most 0.012.
Values may be sent and summed in bfloat16 or wider, within the bound.
A program may use at most 64 MiB of HBM per device.

```python
import math
import jax
import jax.numpy as jnp
import numpy as np
from jax import lax

D = 2048
F = 512
DS = 512
TOP_K = 4
TOK_DEV = 64
EXPERTS = 128
CAP = 3
TOK_A = 8192
TOK_B = 8192
N_EP = 32
N_TP = 4


def block_scale(key, extent, pieces, low, high):
    def one(dim, blocks):
        steps = jax.random.uniform(jax.random.fold_in(jax.random.fold_in(key, 6), dim), (blocks,), jnp.float32, low / len(pieces), high / len(pieces))
        return jnp.repeat(jnp.exp(steps), extent[dim] // blocks).reshape((-1,) + (1,) * (len(extent) - dim - 1))

    gain = one(*pieces[0])
    for cut in pieces[1:]:
        gain = gain * one(*cut)
    return gain


def routed_block(key, own, number, rows, number_of, top, limit, skew):
    sequence = jax.random.permutation(key, number_of)
    packed, common = shares(number_of, rows * top, limit, skew, True), shares(number_of, rows * top, limit, skew, False)
    places = jnp.arange(number_of)

    def named(tallies, offset_by):
        used = int((tallies > 0).sum())
        fixed = max(1, used // 4)
        passed = fixed + (places - fixed + offset_by * (used - fixed)) % max(1, number_of - fixed)
        return jnp.zeros((number_of,), jnp.int32).at[sequence[jnp.where(places < fixed, places, passed)]].set(jnp.asarray(tallies, jnp.int32))

    tallies = jnp.where(number % 4 == 0, named(packed, number // 4), named(common, number - number // 4 - 1))
    mixed = jax.random.permutation(jax.random.fold_in(own, 3), number_of)
    source_of, taker = mixed[0:number_of // 2 * 2:2], mixed[1:number_of // 2 * 2:2]
    room = jnp.minimum(tallies[source_of] - 1, limit - tallies[taker]) // 2
    room = jnp.where((source_of == sequence[0]) | (taker == sequence[0]) | (tallies[taker] == 0), 0, jnp.maximum(room, 0))
    passed = jax.random.randint(jax.random.fold_in(own, 4), (number_of // 2,), 0, 1 << 20) % (room + 1)
    tallies = tallies.at[source_of].add(-passed).at[taker].add(passed)
    labels = jnp.searchsorted(jnp.cumsum(tallies), jnp.arange(rows * top), side="right").astype(jnp.int32)
    listing = labels.reshape(top, rows).T
    listing = listing[jax.random.permutation(jax.random.fold_in(own, 1), rows)]
    offset_by = jax.random.randint(jax.random.fold_in(own, 2), (rows, 1), 0, top)
    return jnp.take_along_axis(listing, (jnp.arange(top)[None, :] + offset_by) % top, axis=1)


def shares(amount, total, bound, slope, full):
    loads = [(1 << 20) // math.isqrt(rank ** slope) + 1 for rank in range(1, amount + 1)]
    largest = bound if full else min(bound, max(-(-total // amount), total * loads[0] // sum(loads)))
    least = 1 if total - largest >= amount - 1 else 0
    given, surplus = [largest] + [least] * (amount - 1), total - largest - least * (amount - 1)
    while surplus > 0:
        movable = [i for i in range(1, amount) if given[i] < largest] or [i for i in range(1, amount) if given[i] < bound]
        mass, remaining = sum([loads[i] for i in movable]), surplus
        for i in movable:
            extra = min(bound - given[i], max(1, remaining * loads[i] // mass), surplus)
            given[i] = given[i] + extra
            surplus = surplus - extra
    return np.array(given)


def centred(key, dims, deviation, bound, shards=(), kind=jnp.bfloat16):
    factor_of = block_scale(key, dims, shards, -0.22, 0.18) if shards else 1.0
    array = jax.random.normal(key, dims, jnp.float32) * deviation * factor_of
    return jnp.minimum(jnp.maximum(array, -bound), bound).astype(kind)


def setup_inputs(seed: int = 0, part: int = 0) -> dict:
    seeds = jax.random.split(jax.random.key(seed), 17)
    part_splits = jax.random.split(jax.random.fold_in(seeds[16], part), 17)
    outer_gate = centred(part_splits[0], (TOK_A, D), 1.0, 6.0, ((0, 32), (1, 4)))
    inner_gate = centred(part_splits[1], (TOK_A, D), 1.0, 6.0, ((0, 32), (1, 4)))
    inner_value = centred(part_splits[2], (TOK_A, D), 1.0, 6.0, ((0, 32), (1, 4)))
    conv_taps = centred(seeds[3], (3, D), 0.577, 3.0)
    mixer_out = centred(seeds[4], (D, D), D ** -0.5, 0.125, ((0, 4),))
    mixer_gain = jnp.clip(1.0 + 0.18 * jax.random.normal(seeds[5], (D,), jnp.float32), 0.1, 1.9)
    moe_tokens = centred(part_splits[6], (TOK_B, D), 1.0, 6.0, ((0, 128),))
    expert_gain = jnp.clip(1.0 + 0.18 * jax.random.normal(seeds[7], (D,), jnp.float32), 0.1, 1.9)
    route_ids_keys = jax.random.split(jax.random.fold_in(part_splits[8], 1), TOK_B // TOK_DEV)
    route_ids_turns = jax.random.permutation(jax.random.fold_in(part_splits[8], 3), TOK_B // TOK_DEV)
    route_ids = jax.vmap(lambda own, number: routed_block(jax.random.fold_in(part_splits[8], 2), own, number, TOK_DEV, EXPERTS, TOP_K, CAP, 2))(route_ids_keys, route_ids_turns).reshape((TOK_B, TOP_K))
    route_weights = jnp.clip(jnp.exp(math.log(1.0) - 1.609438 * jax.random.uniform(part_splits[9], (TOK_B, TOP_K), jnp.float32) ** block_scale(part_splits[9], (TOK_B, TOP_K), ((0, 128),), -0.2, 0.2)), 0.2, 1.0)
    expert_gate = centred(seeds[10], (EXPERTS, D, F), D ** -0.5, 0.125, ((0, 128),))
    expert_up = centred(seeds[11], (EXPERTS, D, F), D ** -0.5, 0.125, ((0, 128),))
    expert_down = centred(seeds[12], (EXPERTS, F, D), F ** -0.5, 0.25, ((0, 128),))
    shared_gate = centred(seeds[13], (D, DS), D ** -0.5, 0.125, ((1, 4),))
    shared_up = centred(seeds[14], (D, DS), D ** -0.5, 0.125, ((1, 4),))
    shared_down = centred(seeds[15], (DS, D), DS ** -0.5, 0.25, ((0, 4),))
    return {"outer_gate": outer_gate, "inner_gate": inner_gate, "inner_value": inner_value, "conv_taps": conv_taps, "mixer_out": mixer_out, "mixer_gain": mixer_gain, "moe_tokens": moe_tokens, "expert_gain": expert_gain, "route_ids": route_ids, "route_weights": route_weights, "expert_gate": expert_gate, "expert_up": expert_up, "expert_down": expert_down, "shared_gate": shared_gate, "shared_up": shared_up, "shared_down": shared_down}


EPSILON = 1e-06

def rms_scale(values, gains):
    return values * lax.rsqrt(lax.optimization_barrier(jnp.mean(values * values, axis=-1, keepdims=True)) + EPSILON) * gains

def reference(outer_gate, inner_gate, inner_value, conv_taps, mixer_out, mixer_gain, moe_tokens, expert_gain, route_ids, route_weights, expert_gate, expert_up, expert_down, shared_gate, shared_up, shared_down):
    kernel = conv_taps.astype(jnp.float32)
    product = inner_gate.astype(jnp.float32) * inner_value.astype(jnp.float32)
    padded = jnp.concatenate([jnp.zeros((2, product.shape[1]), jnp.float32), product], axis=0)
    filtered = kernel[0] * padded[:-2] + kernel[1] * padded[1:-1] + kernel[2] * padded[2:]
    scaled = (outer_gate.astype(jnp.float32) * filtered).astype(jnp.bfloat16)
    shard_width = D // N_TP
    summed = jnp.zeros((scaled.shape[0], D), jnp.float32)
    for shard_index in range(N_TP):
        low = shard_index * shard_width
        partial_sum = jnp.dot(scaled[:, low:low + shard_width], mixer_out[low:low + shard_width], preferred_element_type=jnp.float32)
        rounded = lax.optimization_barrier(partial_sum.astype(jnp.bfloat16))
        summed = summed + rounded.astype(jnp.float32)
    mixed_rows = rms_scale(summed, mixer_gain.astype(jnp.float32)).astype(jnp.bfloat16)
    normed = rms_scale(moe_tokens.astype(jnp.float32), expert_gain.astype(jnp.float32)).astype(jnp.bfloat16)
    token_total = normed.shape[0]
    flat_ids = route_ids.reshape(-1).astype(jnp.int32)
    onehot = (flat_ids[:, None] == jnp.arange(EXPERTS, dtype=jnp.int32)[None, :]).astype(jnp.int32)
    slot_rank = lax.optimization_barrier(jnp.sum((jnp.cumsum(onehot, axis=0, dtype=jnp.int32) - onehot) * onehot, axis=1, dtype=jnp.int32))
    token_of = jnp.arange(flat_ids.shape[0], dtype=jnp.int32) // TOP_K
    slot_count = N_EP * N_TP * CAP
    target = flat_ids * slot_count + slot_rank
    slot_token = jnp.full((EXPERTS * slot_count,), token_total, jnp.int32).at[target].set(token_of).reshape(EXPERTS, slot_count)
    slot_weight = jnp.zeros((EXPERTS * slot_count,), jnp.float32).at[target].set(route_weights.reshape(-1).astype(jnp.float32)).reshape(EXPERTS, slot_count)
    padded_rows = jnp.concatenate([normed, jnp.zeros((1, D), jnp.bfloat16)], axis=0)

    def expert_step(routed, inputs):
        gate_weight, up_weight, down_weight, tokens_here, weights_here = inputs
        chosen = padded_rows[tokens_here]
        gate_value = jnp.dot(chosen, gate_weight, preferred_element_type=jnp.float32)
        up_value = jnp.dot(chosen, up_weight, preferred_element_type=jnp.float32)
        active = (jax.nn.silu(gate_value) * up_value).astype(jnp.bfloat16)
        result = jnp.dot(active, down_weight, preferred_element_type=jnp.float32)
        result = lax.optimization_barrier(result.astype(jnp.bfloat16)).astype(jnp.float32)
        return (routed.at[tokens_here].add(weights_here[:, None] * result), None)
    routed, unused = lax.scan(expert_step, jnp.zeros((token_total + 1, D), jnp.float32), (expert_gate, expert_up, expert_down, slot_token, slot_weight))
    shared_gate_value = jnp.dot(normed, shared_gate, preferred_element_type=jnp.float32)
    shared_up_value = jnp.dot(normed, shared_up, preferred_element_type=jnp.float32)
    shared_act = (jax.nn.silu(shared_gate_value) * shared_up_value).astype(jnp.bfloat16)
    hidden_width = DS // N_TP
    shared_out = jnp.zeros((token_total, D), jnp.float32)
    for shard_index in range(N_TP):
        low = shard_index * hidden_width
        partial_sum = jnp.dot(shared_act[:, low:low + hidden_width], shared_down[low:low + hidden_width], preferred_element_type=jnp.float32)
        rounded = lax.optimization_barrier(partial_sum.astype(jnp.bfloat16))
        shared_out = shared_out + rounded.astype(jnp.float32)
    expert_rows = (routed[:token_total] + shared_out).astype(jnp.bfloat16)
    return (mixed_rows, expert_rows)
```

```python
import functools

import jax
import jax.numpy as jnp
from jax import lax
from jax.experimental import pallas as pl
from jax.experimental.pallas import tpu as pltpu
from jax.sharding import PartitionSpec as P

EPSILON = 1e-06
CAP = 3
PAD = 8
BF = jnp.bfloat16
F32 = jnp.float32
MESH = pl.DeviceIdType.MESH


def scale_of(v):
    return lax.rsqrt(jnp.mean(v * v, axis=-1, keepdims=True) + EPSILON)


def kernel(
    steps,
    tp_count,
    tok_ref,
    egain_ref,
    route_ref,
    taps_ref,
    mgain_ref,
    og_ref,
    ig_ref,
    iv_ref,
    mixw_hbm,
    wg_hbm,
    wu_hbm,
    wd_hbm,
    sg_hbm,
    su_hbm,
    sd_hbm,
    mix_out,
    exp_out,
    mixw,
    wg,
    wu,
    wd,
    sg,
    su,
    sd,
    agbuf,
    rbuf,
    xsend,
    xin,
    act,
    ybuf,
    ret,
    sbuf,
    shi,
    slo,
    cbuf,
    cown,
    rsend,
    rrecv,
    halo,
    scaled,
    part,
    rs_a,
    rs_b,
    xs,
    w_sem,
    d_send,
    d_recv,
    t_send,
    t_recv,
    x_send,
    x_recv,
    y_send,
    y_recv,
    r_send,
    r_recv,
    h_send,
    h_recv,
    g_send,
    g_recv,
    q_send,
    q_recv,
):
    last = steps - 1
    nz = 2 * steps
    me = lax.axis_index("ep")
    t = lax.axis_index("tp")
    c = lax.rem(me, 2)
    z = me // 2
    ep_count = 2 * nz
    up = lax.rem(me + 2, ep_count)
    down = lax.rem(me + ep_count - 2, ep_count)
    up_dev = {"ep": up, "tp": t}
    down_dev = {"ep": down, "tp": t}
    right = {"ep": me, "tp": lax.rem(t + 1, tp_count)}
    left = {"ep": me, "tp": lax.rem(t + tp_count - 1, tp_count)}
    after = {"ep": lax.rem(me + 1, ep_count), "tp": t}
    cross = {"ep": lax.rem(me + ep_count + 2 * c - 1, ep_count), "tp": t}
    j_me = c * tp_count + t
    rows = tok_ref.shape[0]
    half = rows // 2
    width = tok_ref.shape[1]
    plane = 2 * tp_count
    slots = plane * PAD

    peers = []
    for dc in range(2):
        for dt in range(tp_count):
            if dc or dt:
                pc = lax.rem(c + dc, 2)
                pt = lax.rem(t + dt, tp_count)
                peers.append((pc * tp_count + pt, {"ep": 2 * z + pc, "tp": pt}))

    def rcopy(src, dst, ssem, rsem, dev):
        return pltpu.make_async_remote_copy(
            src_ref=src,
            dst_ref=dst,
            send_sem=ssem,
            recv_sem=rsem,
            device_id=dev,
            device_id_type=MESH,
        )

    loads = [
        pltpu.make_async_copy(s, d, w_sem.at[n])
        for n, (s, d) in enumerate(
            (
                (mixw_hbm, mixw),
                (sg_hbm, sg),
                (su_hbm, su),
                (sd_hbm, sd),
                (wg_hbm.at[0], wg),
                (wu_hbm.at[0], wu),
                (wd_hbm.at[0], wd),
            )
        )
    ]
    for load in loads:
        load.start()

    barrier = pltpu.get_barrier_semaphore()
    greeted = [up_dev, down_dev, cross] + [dev for _, dev in peers]
    for dev in greeted:
        pl.semaphore_signal(barrier, inc=1, device_id=dev, device_id_type=MESH)

    tok = tok_ref[...].astype(F32)
    agbuf[last, rows : 2 * rows, :] = (tok * scale_of(tok) * egain_ref[...]).astype(BF)
    rbuf[last, 1] = route_ref[...]
    pl.semaphore_wait(barrier, len(greeted))

    own = agbuf.at[last, pl.ds(rows, rows)]

    def ring_rows(way, h):
        return pl.ds(way * rows + h * half, half)

    ways = (up_dev, down_dev)

    def first_send(way, h):
        return rcopy(
            agbuf.at[last, pl.ds(rows + h * half, half)],
            agbuf.at[0, ring_rows(way, h)],
            d_send.at[way, h, 0],
            d_recv.at[way, h, 0],
            ways[way],
        )

    def ring_send(way, h, i):
        return rcopy(
            agbuf.at[i, ring_rows(way, h)],
            agbuf.at[i + 1, ring_rows(way, h)],
            d_send.at[way, h, i + 1],
            d_recv.at[way, h, i + 1],
            ways[way],
        )

    def last_send(way):
        return rcopy(
            agbuf.at[last - 1, ring_rows(way, way)],
            agbuf.at[last, pl.ds(way * half, half)],
            d_send.at[way, way, last],
            d_recv.at[way, way, last],
            ways[way],
        )

    def route_send(way, i):
        return rcopy(
            rbuf.at[i, way], rbuf.at[i + 1, way], t_send.at[way, i + 1], t_recv.at[way, i + 1], ways[way]
        )

    def route_first(way):
        return rcopy(
            rbuf.at[last, 1], rbuf.at[0, way], t_send.at[way, 0], t_recv.at[way, 0], ways[way]
        )

    for h in range(2):
        for way in range(2):
            first_send(way, h).start()
        if h == 0:
            for way in range(2):
                route_first(way).start()

    edge = ig_ref.shape[0] - 16
    halo_sends = [
        rcopy(src.at[pl.ds(edge, 16)], halo.at[n], h_send.at[n], h_recv.at[n], after)
        for n, src in enumerate((ig_ref, iv_ref))
    ]
    for s in halo_sends:
        s.start()
    gather = [
        rcopy(own, xs.at[3], g_send.at[0], g_recv.at[0], right),
        rcopy(own, xs.at[1], g_send.at[1], g_recv.at[1], left),
        rcopy(
            xs.at[3, pl.ds(0, half)], xs.at[2, pl.ds(0, half)], g_send.at[2], g_recv.at[2], right
        ),
        rcopy(
            xs.at[1, pl.ds(half, half)],
            xs.at[2, pl.ds(half, half)],
            g_send.at[3],
            g_recv.at[3],
            left,
        ),
    ]
    gather[0].start()
    gather[1].start()

    def block(k):
        return lax.rem(t + k, tp_count)

    def scatter_one(which):
        return [
            rcopy(
                part.at[which, block(2), pl.ds(0, half)],
                rs_a.at[which, 0],
                q_send.at[which, 0],
                q_recv.at[which, 0],
                right,
            ),
            rcopy(
                part.at[which, block(2), pl.ds(half, half)],
                rs_a.at[which, 1],
                q_send.at[which, 1],
                q_recv.at[which, 1],
                left,
            ),
            rcopy(
                part.at[which, block(1), pl.ds(half, half)],
                rs_b.at[which, 0, pl.ds(half, half)],
                q_send.at[which, 2],
                q_recv.at[which, 2],
                right,
            ),
            rcopy(
                part.at[which, block(3), pl.ds(0, half)],
                rs_b.at[which, 1, pl.ds(0, half)],
                q_send.at[which, 3],
                q_recv.at[which, 3],
                left,
            ),
        ]

    def scatter_two(which):
        return [
            rcopy(
                part.at[which, block(1), pl.ds(0, half)],
                rs_b.at[which, 0, pl.ds(0, half)],
                q_send.at[which, 4],
                q_recv.at[which, 4],
                right,
            ),
            rcopy(
                part.at[which, block(3), pl.ds(half, half)],
                rs_b.at[which, 1, pl.ds(half, half)],
                q_send.at[which, 5],
                q_recv.at[which, 5],
                left,
            ),
        ]

    def start_scatter(which):
        for s in scatter_one(which):
            s.start()

    def go_on_scatter(which):
        one, two = scatter_one(which), scatter_two(which)
        for n, (k, r) in enumerate(((1, 0), (3, half))):
            one[n].wait_recv()
            at = (which, block(k), pl.ds(r, half))
            part[at] = (part[at].astype(F32) + rs_a[which, n].astype(F32)).astype(BF)
            two[n].start()

    def end_scatter(which):
        one, two = scatter_one(which), scatter_two(which)
        for s in (one[2], one[3], two[0], two[1]):
            s.wait_recv()
        return (
            part[which, t].astype(F32)
            + rs_b[which, 0].astype(F32)
            + rs_b[which, 1].astype(F32)
        )

    def mixer():
        columns = ig_ref.shape[1]
        taps = taps_ref[:, pl.ds(pl.multiple_of(t * columns, columns), columns)].astype(F32)
        for s in halo_sends:
            s.wait_recv()
        ahead = halo[0].astype(F32) * halo[1].astype(F32)
        ahead = jnp.where(me > 0, ahead, 0.0)
        product = ig_ref[...].astype(F32) * iv_ref[...].astype(F32)
        number = lax.broadcasted_iota(jnp.int32, product.shape, 0)
        one = jnp.where(number == 0, ahead[15:16], pltpu.roll(product, 1, 0))
        two = pltpu.roll(product, 2, 0)
        two = jnp.where(number == 0, ahead[14:15], jnp.where(number == 1, ahead[15:16], two))
        filtered = taps[0:1] * two + taps[1:2] * one + taps[2:3] * product
        scaled[...] = (og_ref[...].astype(F32) * filtered).astype(BF)
        loads[0].wait()

        @pl.loop(0, tp_count)
        def _(b):
            lhs = scaled[pl.ds(pl.multiple_of(b * rows, rows), rows), :]
            for n in range(width // 512):
                at = pl.ds(n * 512, 512)
                part[0, b, :, at] = jnp.dot(
                    lhs, mixw[:, at], preferred_element_type=F32
                ).astype(BF)

    def shared():
        gather[2].wait_recv()
        gather[3].wait_recv()
        for n in (1, 2, 3):
            loads[n].wait()

        @pl.loop(0, tp_count)
        def _(k):
            b = block(k)
            lhs = xs[k]
            gate = jnp.dot(lhs, sg[...], preferred_element_type=F32)
            upper = jnp.dot(lhs, su[...], preferred_element_type=F32)
            hidden = (jax.nn.silu(gate) * upper).astype(BF)
            for n in range(width // 512):
                at = pl.ds(n * 512, 512)
                part[1, b, :, at] = jnp.dot(
                    hidden, sd[:, at], preferred_element_type=F32
                ).astype(BF)

    def select(i):
        lane = lax.broadcasted_iota(jnp.int32, (PAD, 2 * rows), 1)
        route = jnp.where(lane < rows, rbuf[i, 0], rbuf[i, 1])
        row = lax.broadcasted_iota(jnp.int32, (slots, 2 * rows), 0)
        col = lax.broadcasted_iota(jnp.int32, (slots, 2 * rows), 1)
        place = lax.rem(row, PAD)
        expert = (z * plane + row // PAD).astype(F32)
        hit = jnp.zeros((slots, 2 * rows), F32)
        weight = jnp.zeros((slots, 2 * rows), F32)
        for k in range(4):
            same = expert == route[k : k + 1]
            hit = jnp.where(same, 1.0, hit)
            weight = jnp.where(same, route[4 + k : 5 + k], weight)
        side = (place // CAP) == (col // rows)
        hit = jnp.where(side, hit, 0.0)
        order = lax.broadcasted_iota(jnp.int32, (2 * rows, 2 * rows), 0)
        later = lax.broadcasted_iota(jnp.int32, (2 * rows, 2 * rows), 1)
        below = jnp.where(order < later, 1.0, 0.0).astype(BF)
        rank = jnp.dot(hit.astype(BF), below, preferred_element_type=F32)
        hit = jnp.where(rank == lax.rem(place, CAP).astype(F32), hit, 0.0)
        weight = weight * hit
        high = weight.astype(BF)
        shi[i] = high
        slo[i] = (weight - high.astype(F32)).astype(BF)
        sbuf[...] = hit.astype(BF)
        for n in range(width // 512):
            at = pl.ds(n * 512, 512)
            got = jnp.dot(sbuf[...], agbuf[i, :, at], preferred_element_type=F32)
            xsend[i, :, :, at] = got.reshape(plane, PAD, 512).astype(BF)
        xin[i, j_me] = xsend[i, j_me]
        for j, dev in peers:
            rcopy(xsend.at[i, j], xin.at[i, j_me], x_send.at[i], x_recv.at[i], dev).start()

    def all_peers(buf, i, sem):
        ref = buf.at[i, pl.ds(0, plane - 1)]
        return pltpu.make_async_copy(ref, ref, sem.at[i])

    def expert(i):
        all_peers(xin, i, x_recv).wait()
        lhs = xin[i].reshape(slots, width)
        for n in range(act.shape[1] // 256):
            at = pl.ds(n * 256, 256)
            gate = jnp.dot(lhs, wg[:, at], preferred_element_type=F32)
            upper = jnp.dot(lhs, wu[:, at], preferred_element_type=F32)
            act[:, at] = (jax.nn.silu(gate) * upper).astype(BF)
        for n in range(width // 512):
            at = pl.ds(n * 512, 512)
            got = jnp.dot(act[...], wd[:, at], preferred_element_type=F32)
            ybuf[i, :, :, at] = got.reshape(plane, PAD, 512).astype(BF)

    def give_back(i):
        ret[i, j_me] = ybuf[i, j_me]
        for j, dev in peers:
            rcopy(ybuf.at[i, j], ret.at[i, j_me], y_send.at[i], y_recv.at[i], dev).start()

    mixer()
    start_scatter(0)
    for n in (4, 5, 6):
        loads[n].wait()

    @pl.loop(0, steps)
    def _(i):
        for h in range(2):
            for way in range(2):

                @pl.when(i < last)
                def _():
                    rcopy(
                        agbuf.at[i, ring_rows(way, h)],
                        agbuf.at[i, ring_rows(way, h)],
                        d_send.at[way, h, i],
                        d_recv.at[way, h, i],
                        ways[way],
                    ).wait_recv()

                @pl.when(i < last - 1)
                def _():
                    ring_send(way, h, i).start()

                if h == way:

                    @pl.when(i == last - 1)
                    def _():
                        last_send(way).start()

                    @pl.when(i == last)
                    def _():
                        last_send(way).wait_recv()

            if h == 0:
                for way in range(2):

                    @pl.when(i < last)
                    def _():
                        rcopy(
                            rbuf.at[i, way],
                            rbuf.at[i, way],
                            t_send.at[way, i],
                            t_recv.at[way, i],
                            ways[way],
                        ).wait_recv()

                    @pl.when(i < last - 1)
                    def _():
                        route_send(way, i).start()

                @pl.when(i == last - 1)
                def _():
                    route_send(0, i).start()

                @pl.when(i == last)
                def _():
                    rcopy(
                        rbuf.at[i, 0], rbuf.at[i, 0], t_send.at[0, i], t_recv.at[0, i], ways[0]
                    ).wait_recv()

                @pl.when(i == 0)
                def _():
                    xs[0] = own[...]
                    gather[0].wait_recv()
                    gather[2].start()
                    gather[1].wait_recv()
                    gather[3].start()

                @pl.when(i == 1)
                def _():
                    shared()

                @pl.when(i >= 2)
                def _():
                    expert(i - 2)

                @pl.when(i == 2)
                def _():
                    go_on_scatter(0)

        select(i)

    expert(last - 1)
    expert(last)
    give_back(last)
    give_back(last - 1)
    give_back(last - 2)

    def combine(i, slot):
        all_peers(ret, i, y_recv).wait()
        for n in range(width // 512):
            at = pl.ds(n * 512, 512)
            rhs = ret[i, :, :, at].reshape(slots, 512)
            turn = (((0,), (0,)), ((), ()))
            got = lax.dot_general(shi[i], rhs, turn, preferred_element_type=F32)
            got += lax.dot_general(slo[i], rhs, turn, preferred_element_type=F32)
            cbuf[slot, :, at] = got

    back = (down_dev, up_dev)

    def back_send(way, h, i):
        return rcopy(
            rsend.at[i, ring_rows(way, h)],
            rrecv.at[i, ring_rows(way, h)],
            r_send.at[way, h, i],
            r_recv.at[way, h, i],
            back[way],
        )

    def back_last(way):
        return rcopy(
            rsend.at[last, pl.ds(way * half, half)],
            rrecv.at[last, ring_rows(way, way)],
            r_send.at[way, way, last],
            r_recv.at[way, way, last],
            back[way],
        )

    combine(last, 0)
    for way in range(2):
        at = pl.ds(way * half, half)
        rsend[last, at] = cbuf[0, at].astype(BF)
        back_last(way).start()
    cown[...] = cbuf[0, rows : 2 * rows]
    combine(last - 1, 1)

    @pl.loop(0, last)
    def _(n):
        i = last - 1 - n
        slot = lax.rem(n + 1, 2)

        @pl.when(i >= 2)
        def _():
            give_back(i - 2)

        for h in range(2):
            for way in range(2):
                at = ring_rows(way, h)
                if h == way:

                    @pl.when(i == last - 1)
                    def _():
                        back_last(way).wait_recv()

                @pl.when(i < last - 1)
                def _():
                    back_send(way, h, i + 1).wait_recv()

                if h == way:
                    total = cbuf[slot, at] + rrecv[i + 1, at].astype(F32)
                    rsend[i, at] = total.astype(BF)
                else:

                    @pl.when(i < last - 1)
                    def _():
                        total = cbuf[slot, at] + rrecv[i + 1, at].astype(F32)
                        rsend[i, at] = total.astype(BF)

                    @pl.when(i == last - 1)
                    def _():
                        rsend[i, at] = cbuf[slot, at].astype(BF)

                back_send(way, h, i).start()
            if h == 0:

                @pl.when(i > 0)
                def _():
                    combine(i - 1, 1 - slot)

        @pl.when(n == 1)
        def _():
            start_scatter(1)

        @pl.when(n == 3)
        def _():
            go_on_scatter(1)

    mixed = end_scatter(0)
    mix_out[...] = (mixed * scale_of(mixed) * mgain_ref[...]).astype(BF)
    cown[...] = cown[...] + end_scatter(1)
    for h in range(2):
        for way in range(2):
            back_send(way, h, 0).wait_recv()
    exp_out[...] = (
        cown[...] + rrecv[0, 0:rows].astype(F32) + rrecv[0, rows : 2 * rows].astype(F32)
    ).astype(BF)

    for s in halo_sends + gather:
        s.wait_send()
    for which in range(2):
        for s in scatter_one(which) + scatter_two(which):
            s.wait_send()
    for way in range(2):
        last_send(way).wait_send()
        back_last(way).wait_send()
    route_send(0, last - 1).wait_send()

    @pl.loop(0, steps)
    def _(i):
        all_peers(xin, i, x_send).wait()
        all_peers(xin, i, y_send).wait()

        @pl.when(i < last)
        def _():
            for way in range(2):
                rcopy(
                    rbuf.at[i, way], rbuf.at[i, way], t_send.at[way, i], t_recv.at[way, i], ways[way]
                ).wait_send()
                for h in range(2):
                    rcopy(
                        agbuf.at[i, ring_rows(way, h)],
                        agbuf.at[i, ring_rows(way, h)],
                        d_send.at[way, h, i],
                        d_recv.at[way, h, i],
                        ways[way],
                    ).wait_send()
                    back_send(way, h, i).wait_send()


def on_device(
    outer_gate,
    inner_gate,
    inner_value,
    conv_taps,
    mixer_out,
    mixer_gain,
    moe_tokens,
    expert_gain,
    route_ids,
    route_weights,
    expert_gate,
    expert_up,
    expert_down,
    shared_gate,
    shared_up,
    shared_down,
):
    ep_count = lax.axis_size("ep")
    tp_count = lax.axis_size("tp")
    steps = ep_count // 4
    plane = 2 * tp_count
    rows, width = moe_tokens.shape
    half = rows // 2
    hidden = expert_gate.shape[2]
    route = jnp.concatenate([route_ids.astype(F32).T, route_weights.T], axis=0)
    route = jnp.concatenate([route, route], axis=1)
    vm = pl.BlockSpec(memory_space=pltpu.VMEM)
    hbm = pl.BlockSpec(memory_space=pl.ANY)
    dma = pltpu.SemaphoreType.DMA
    scratch = [
        pltpu.VMEM(mixer_out.shape, BF),
        pltpu.VMEM(expert_gate.shape[1:], BF),
        pltpu.VMEM(expert_up.shape[1:], BF),
        pltpu.VMEM(expert_down.shape[1:], BF),
        pltpu.VMEM(shared_gate.shape, BF),
        pltpu.VMEM(shared_up.shape, BF),
        pltpu.VMEM(shared_down.shape, BF),
        pltpu.VMEM((steps, 2 * rows, width), BF),
        pltpu.VMEM((steps, 2, PAD, 2 * rows), F32),
        pltpu.VMEM((steps, plane, PAD, width), BF),
        pltpu.VMEM((steps, plane, PAD, width), BF),
        pltpu.VMEM((plane * PAD, hidden), BF),
        pltpu.VMEM((steps, plane, PAD, width), BF),
        pltpu.VMEM((steps, plane, PAD, width), BF),
        pltpu.VMEM((plane * PAD, 2 * rows), BF),
        pltpu.VMEM((steps, plane * PAD, 2 * rows), BF),
        pltpu.VMEM((steps, plane * PAD, 2 * rows), BF),
        pltpu.VMEM((2, 2 * rows, width), F32),
        pltpu.VMEM((rows, width), F32),
        pltpu.VMEM((steps, 2 * rows, width), BF),
        pltpu.VMEM((steps, 2 * rows, width), BF),
        pltpu.VMEM((2, 16, inner_gate.shape[1]), BF),
        pltpu.VMEM(inner_gate.shape, BF),
        pltpu.VMEM((2, tp_count, rows, width), BF),
        pltpu.VMEM((2, 2, half, width), BF),
        pltpu.VMEM((2, 2, rows, width), BF),
        pltpu.VMEM((tp_count, rows, width), BF),
        dma((7,)),
        dma((2, 2, steps)),
        dma((2, 2, steps)),
        dma((2, steps)),
        dma((2, steps)),
        dma((steps,)),
        dma((steps,)),
        dma((steps,)),
        dma((steps,)),
        dma((2, 2, steps)),
        dma((2, 2, steps)),
        dma((2,)),
        dma((2,)),
        dma((4,)),
        dma((4,)),
        dma((2, 6)),
        dma((2, 6)),
    ]
    out = jax.ShapeDtypeStruct((rows, width), BF)
    return pl.pallas_call(
        functools.partial(kernel, steps, tp_count),
        out_shape=(out, out),
        in_specs=[vm] * 8 + [hbm] * 7,
        out_specs=(vm, vm),
        scratch_shapes=scratch,
        compiler_params=pltpu.CompilerParams(
            collective_id=0, has_side_effects=True, vmem_limit_bytes=60 * 1024 * 1024
        ),
        name="layer",
    )(
        moe_tokens,
        expert_gain.reshape(1, -1),
        route,
        conv_taps,
        mixer_gain.reshape(1, -1),
        outer_gate,
        inner_gate,
        inner_value,
        mixer_out,
        expert_gate,
        expert_up,
        expert_down,
        shared_gate,
        shared_up,
        shared_down,
    )


def solution(mesh):
    return jax.shard_map(
        on_device,
        mesh=mesh,
        in_specs=(
            P(("grp", "ep"), "tp"),
            P(("grp", "ep"), "tp"),
            P(("grp", "ep"), "tp"),
            P(),
            P("tp", None),
            P(),
            P(("grp", "ep", "tp"), None),
            P(),
            P(("grp", "ep", "tp"), None),
            P(("grp", "ep", "tp"), None),
            P(("ep", "tp"), None, None),
            P(("ep", "tp"), None, None),
            P(("ep", "tp"), None, None),
            P(None, "tp"),
            P(None, "tp"),
            P("tp", None),
        ),
        out_specs=(P(("grp", "ep", "tp"), None), P(("grp", "ep", "tp"), None)),
        check_vma=False,
    )
```
